32 devices in a mesh: rep: 2 (over x), fs: 8 (over z, y), tp: 2 (over core).
Axes of the slice: x: 2, y: 2, z: 4, core: 2. Of those that a mesh axis runs over, the one named last changes fastest.
Arguments:
- x_later: bfloat16 [2048, 2048], P(('rep', 'fs')), may hold values from -6 to 6
- kept_input_rows: bfloat16 [2048, 2048], P(('rep', 'fs')), may hold values from -6 to 6
- cotangent: bfloat16 [2048, 2048], P(('rep', 'fs')), may hold values from -8 to 8
- norm_gain_vector: float32 [2048], replicated, may hold values from 0.1 to 1.9
- up_weight: bfloat16 [2048, 4096], P('fs', 'tp'), may hold values from -0.125 to 0.125
- down_weight: bfloat16 [4096, 2048], P('tp', 'fs'), may hold values from -0.09375 to 0.09375
- up_sum: float32 [2048, 4096], P('fs', 'tp'), may hold values from -6 to 6
- down_sum: float32 [4096, 2048], P('tp', 'fs'), may hold values from -6 to 6
Outputs:
- mixed: bfloat16 [2048, 2048], P(('rep', 'fs'))
- input_gradient_rows: bfloat16 [2048, 2048], P(('rep', 'fs'))
- up_total: float32 [2048, 4096], P('fs', 'tp')
- down_total: float32 [4096, 2048], P('tp', 'fs')
The draws below stay inside these ranges and needn't reach their ends.
All inputs are finite; a program needn't handle non-finite values.
Results may differ from the reference program's by a relative error of at most 0.018.
Values may be sent and summed in bfloat16 or wider, within the bound.
A program may use at most 128 MiB of HBM per device.

```python
import jax
import jax.numpy as jnp
from jax import lax

D = 2048
FF = 4096
TOKENS = 2048
N_TP = 2


def with_spikes(values, own_key, source, target, shards_of, factor):
    def block_of(dim):
        return (jnp.arange(values.shape[dim]) // (values.shape[dim] // shards_of)).reshape((-1,) + (1,) * (values.ndim - 1 - dim))

    one_side = jax.random.permutation(own_key, shards_of)[block_of(target)]
    far = (block_of(target) + shards_of // 2) % shards_of
    return jnp.where((block_of(source) == one_side) | (block_of(source) == far), factor * values, values)


def block_scale(stream_key, extent, cuts, least, top_value):
    gain, own = 1.0, jax.random.fold_in(stream_key, 6)
    for position, blocks in cuts:
        draws = jnp.exp(jax.random.uniform(jax.random.fold_in(own, position), (blocks,), jnp.float32, least / len(cuts), top_value / len(cuts)))
        gain = gain * jnp.repeat(draws, extent[position] // blocks).reshape([-1 if axis == position else 1 for axis in range(len(extent))])
    return gain


def bell_draw(key, shape, scale, most, cuts=(), kind=jnp.bfloat16):
    entries = scale * jax.random.normal(key, shape, jnp.float32)
    if cuts:
        entries = entries * block_scale(key, shape, cuts, -0.22, 0.18)
    return jnp.clip(entries, -most, most).astype(kind)


def gaussian_with(stream_key, dims, scale, limit, pieces, heavy, held_as=jnp.bfloat16):
    entries = scale * jax.random.normal(stream_key, dims, jnp.float32)
    if pieces:
        entries = entries * block_scale(stream_key, dims, pieces, -0.22, 0.18)
    return jnp.clip(with_spikes(entries, jax.random.fold_in(stream_key, 3), *heavy), -limit, limit).astype(held_as)


def setup_inputs(seed: int = 0) -> dict:
    key_list = jax.random.split(jax.random.key(seed), 9)
    return {
        "x_later": bell_draw(key_list[0], (TOKENS, D), 1.0, 6.0, ((0, 16),)),
        "kept_input_rows": bell_draw(key_list[1], (TOKENS, D), 1.0, 6.0, ((0, 16),)),
        "cotangent": gaussian_with(key_list[2], (TOKENS, D), 1.0, 8.0, ((0, 16),), (0, 1, 16, 2.0)),
        "norm_gain_vector": jnp.clip(1.0 + 0.18 * jax.random.normal(key_list[3], (D,), jnp.float32), 0.1, 1.9),
        "up_weight": bell_draw(key_list[4], (D, FF), D ** -0.5, 0.125, ((0, 8), (1, 2))),
        "down_weight": bell_draw(key_list[5], (FF, D), FF ** -0.5, 0.09375, ((0, 2), (1, 8))),
        "up_sum": bell_draw(key_list[6], (D, FF), 1.0, 6.0, ((0, 8), (1, 2)), jnp.float32),
        "down_sum": bell_draw(key_list[7], (FF, D), 1.0, 6.0, ((0, 2), (1, 8)), jnp.float32),
    }


EPSILON = 1e-06

def norm_partial_terms(values, norm_gain_vector):
    floats = values.astype(jnp.float32)
    inverse = lax.rsqrt(lax.optimization_barrier(jnp.mean(floats * floats, axis=-1, keepdims=True)) + EPSILON)
    unit_rows = floats * inverse
    normed = (unit_rows * norm_gain_vector).astype(jnp.bfloat16)
    return (inverse, unit_rows, normed)

def block_sum(left, right_weight, transpose_right):
    width = FF // N_TP
    result = jnp.zeros((left.shape[0], D), jnp.float32)
    for block in range(N_TP):
        left_block = left[:, block * width:(block + 1) * width]
        if transpose_right:
            part = jnp.dot(left_block, right_weight[:, block * width:(block + 1) * width].T, preferred_element_type=jnp.float32)
        else:
            part = jnp.dot(left_block, right_weight[block * width:(block + 1) * width], preferred_element_type=jnp.float32)
        rounded = lax.optimization_barrier(part.astype(jnp.bfloat16))
        result = result + rounded.astype(jnp.float32)
    return result

def reference(x_later, kept_input_rows, cotangent, norm_gain_vector, up_weight, down_weight, up_sum, down_sum):
    inv_later, unit_later, normed_later = norm_partial_terms(x_later, norm_gain_vector)
    inverse_rms_kept, unit_kept_rows, normed_kept_rows = norm_partial_terms(kept_input_rows, norm_gain_vector)
    pre_later = jnp.dot(normed_later, up_weight, preferred_element_type=jnp.float32)
    pre_saved = jnp.dot(normed_kept_rows, up_weight, preferred_element_type=jnp.float32)
    hidden_later = jnp.square(jax.nn.relu(pre_later)).astype(jnp.bfloat16)
    hidden_saved = jnp.square(jax.nn.relu(pre_saved)).astype(jnp.bfloat16)
    mixed = block_sum(hidden_later, down_weight, False).astype(jnp.bfloat16)
    hidden_grad = jnp.dot(cotangent, down_weight.T, preferred_element_type=jnp.float32)
    pre_grad = (hidden_grad * 2.0 * jax.nn.relu(pre_saved)).astype(jnp.bfloat16)
    normed_grad = block_sum(pre_grad, up_weight, True)
    scaled_rows = normed_grad * norm_gain_vector
    input_gradient_rows = (inverse_rms_kept * (scaled_rows - unit_kept_rows * lax.optimization_barrier(jnp.mean(scaled_rows * unit_kept_rows, axis=-1, keepdims=True)))).astype(jnp.bfloat16)
    grad_scale = TOKENS ** (-0.5)
    up_total = up_sum + grad_scale * jnp.dot(normed_kept_rows.T, pre_grad, preferred_element_type=jnp.float32)
    down_total = down_sum + grad_scale * jnp.dot(hidden_saved.T, cotangent, preferred_element_type=jnp.float32)
    return (mixed, input_gradient_rows, up_total, down_total)
```

```python
import jax
import jax.numpy as jnp
from jax import lax
from jax.sharding import PartitionSpec as P

EPSILON = 1e-06
TRANSPOSED = (((1,), (1,)), ((), ()))
LEADING = (((0,), (0,)), ((), ()))


def norm_partial_terms(values, norm_gain_vector):
    floats = values.astype(jnp.float32)
    inverse = lax.rsqrt(jnp.mean(floats * floats, axis=-1, keepdims=True) + EPSILON)
    unit_rows = floats * inverse
    normed = (unit_rows * norm_gain_vector).astype(jnp.bfloat16)
    return (inverse, unit_rows, normed)


def squared_relu(pre_act):
    return jnp.square(jax.nn.relu(pre_act)).astype(jnp.bfloat16)


def body(
    x_later, kept_input_rows, cotangent, norm_gain_vector, up_weight, down_weight, up_sum, down_sum
):
    row_count = x_later.shape[0]
    grad_scale = float(row_count * lax.axis_size("rep") * lax.axis_size("fs")) ** (-0.5)
    inv_later, unit_later, normed_later = norm_partial_terms(x_later, norm_gain_vector)
    inverse_rms_kept, unit_kept_rows, normed_kept_rows = norm_partial_terms(
        kept_input_rows, norm_gain_vector
    )
    stacked = jnp.concatenate([normed_kept_rows, normed_later], axis=0)
    up_whole = lax.all_gather(up_weight, "fs", axis=0, tiled=True)
    down_whole = lax.all_gather(down_weight, "fs", axis=1, tiled=True)
    pre_act = jnp.dot(stacked, up_whole, preferred_element_type=jnp.float32)
    pre_saved = pre_act[:row_count]
    hidden_saved = squared_relu(pre_saved)
    hidden_later = squared_relu(pre_act[row_count:])
    mixed_part = jnp.dot(hidden_later, down_whole, preferred_element_type=jnp.float32)
    hidden_grad = lax.dot_general(
        cotangent, down_whole, TRANSPOSED, preferred_element_type=jnp.float32
    )
    pre_grad = (hidden_grad * 2.0 * jax.nn.relu(pre_saved)).astype(jnp.bfloat16)
    back_part = lax.dot_general(pre_grad, up_whole, TRANSPOSED, preferred_element_type=jnp.float32)
    mixed_sum, back_sum = (
        lax.psum(mixed_part.astype(jnp.bfloat16), "tp").astype(jnp.float32),
        lax.psum(back_part.astype(jnp.bfloat16), "tp").astype(jnp.float32),
    )
    mixed = mixed_sum.astype(jnp.bfloat16)
    scaled_rows = back_sum * norm_gain_vector
    input_gradient_rows = (
        inverse_rms_kept
        * (
            scaled_rows
            - unit_kept_rows * jnp.mean(scaled_rows * unit_kept_rows, axis=-1, keepdims=True)
        )
    ).astype(jnp.bfloat16)
    cot_columns, normed_columns = (
        lax.all_to_all(cotangent, "fs", split_axis=1, concat_axis=0, tiled=True),
        lax.all_to_all(normed_kept_rows, "fs", split_axis=1, concat_axis=0, tiled=True),
    )
    columns = normed_columns
    up_grad = grad_scale * lax.dot_general(
        columns,
        lax.all_gather(pre_grad, "fs", axis=0, tiled=True),
        LEADING,
        preferred_element_type=jnp.float32,
    )
    columns = cot_columns
    down_grad = lax.dot_general(
        lax.all_gather(hidden_saved, "fs", axis=0, tiled=True),
        columns,
        LEADING,
        preferred_element_type=jnp.float32,
    )
    up_added, down_added = (
        lax.psum(up_grad.astype(jnp.bfloat16), "rep").astype(jnp.float32),
        lax.psum((down_grad * grad_scale).astype(jnp.bfloat16), "rep").astype(jnp.float32),
    )
    return (mixed, input_gradient_rows, up_sum + up_added, down_sum + down_added)


def swap(values, axis):
    size = lax.axis_size(axis)
    return lax.ppermute(values, axis, [(i, i ^ 1) for i in range(size)])


def own_half(values, axis_index, dim):
    return lax.dynamic_index_in_dim(values, axis_index, dim, keepdims=False)


def line_shift(values, shift):
    size = lax.axis_size("fs")
    outer = size // 2
    return lax.ppermute(
        values, "fs", [(i, ((i // 2 + shift) % outer) * 2 + i % 2) for i in range(size)]
    )


def ordered(first, second, axis_index):
    return jnp.where(axis_index == 0, jnp.stack([first, second]), jnp.stack([second, first]))


def gather_tokens(values):
    rows, width = values.shape
    outer = lax.axis_size("fs") // 2
    half = own_half(values.reshape(2, rows // 2, width), lax.axis_index("tp"), 0)
    line = jnp.stack([half] + [line_shift(half, s) for s in range(1, outer)])
    both = jnp.stack([line, swap(line, "fs")])
    return jnp.stack([both, swap(both, "tp")]).reshape(-1, width)


def scatter_tokens(partial, rows):
    width = partial.shape[1]
    outer = lax.axis_size("fs") // 2
    blocks = partial.reshape(2, 2, outer, rows // 2, width)
    got = swap(blocks[1], "tp")
    blocks = (blocks[0].astype(jnp.float32) + got.astype(jnp.float32)).astype(jnp.bfloat16)
    got = swap(blocks[1], "fs")
    blocks = (blocks[0].astype(jnp.float32) + got.astype(jnp.float32)).astype(jnp.bfloat16)
    total = blocks[0].astype(jnp.float32)
    for s in range(1, outer):
        total = total + line_shift(blocks[s], -s).astype(jnp.float32)
    half = total.astype(jnp.bfloat16)
    whole = ordered(half, swap(half, "tp"), lax.axis_index("tp"))
    return whole.reshape(rows, width).astype(jnp.float32)


def hidden_body(
    x_later, kept_input_rows, cotangent, norm_gain_vector, up_weight, down_weight, up_sum, down_sum
):
    row_count, width = x_later.shape
    n_fs = lax.axis_size("fs")
    grad_scale = float(row_count * lax.axis_size("rep") * n_fs) ** (-0.5)
    group = lax.axis_index("rep")
    depth, units = up_weight.shape
    own_units = units // n_fs
    inv_later, unit_later, normed_later = norm_partial_terms(x_later, norm_gain_vector)
    inverse_rms_kept, unit_kept_rows, normed_kept_rows = norm_partial_terms(
        kept_input_rows, norm_gain_vector
    )
    part = own_units // 2
    up_half = own_half(up_weight.reshape(depth, n_fs, 2, part), group, 2)
    down_half = own_half(down_weight.reshape(n_fs, 2, part, depth), group, 1)
    up_half = lax.all_to_all(up_half.transpose(1, 0, 2), "fs", 0, 0, tiled=True)
    down_half = lax.all_to_all(down_half, "fs", 0, 0, tiled=True)
    up_half = up_half.reshape(width, part)
    down_half = down_half.transpose(1, 0, 2).reshape(part, width)
    up_own = jnp.concatenate([up_half, swap(up_half, "rep")], axis=1)
    down_own = jnp.concatenate([down_half, swap(down_half, "rep")], axis=0)

    normed_saved = gather_tokens(normed_kept_rows)
    cot = gather_tokens(cotangent)
    normed_next = gather_tokens(normed_later)

    pre_saved = jnp.dot(normed_saved, up_own, preferred_element_type=jnp.float32)
    hidden_saved = squared_relu(pre_saved)
    hidden_grad = lax.dot_general(cot, down_own, TRANSPOSED, preferred_element_type=jnp.float32)
    pre_grad = (hidden_grad * 2.0 * jax.nn.relu(pre_saved)).astype(jnp.bfloat16)
    up_grad = grad_scale * lax.dot_general(
        normed_saved, pre_grad, LEADING, preferred_element_type=jnp.float32
    )
    down_grad = grad_scale * lax.dot_general(
        hidden_saved, cot, LEADING, preferred_element_type=jnp.float32
    )
    up_got = swap(up_grad[:, part:].astype(jnp.bfloat16), "rep")
    down_got = swap(down_grad[part:].astype(jnp.bfloat16), "rep")
    back_part = lax.dot_general(pre_grad, up_own, TRANSPOSED, preferred_element_type=jnp.float32)
    hidden_later = squared_relu(
        jnp.dot(normed_next, up_own, preferred_element_type=jnp.float32)
    )
    mixed_part = jnp.dot(hidden_later, down_own, preferred_element_type=jnp.float32)
    up_half = (up_grad[:, :part] + up_got.astype(jnp.float32)).astype(jnp.bfloat16)
    down_half = (down_grad[:part] + down_got.astype(jnp.float32)).astype(jnp.bfloat16)
    up_half = lax.all_to_all(up_half.reshape(n_fs, depth, part), "fs", 0, 0, tiled=True)
    down_half = down_half.reshape(part, n_fs, depth).transpose(1, 0, 2)
    down_half = lax.all_to_all(down_half, "fs", 0, 0, tiled=True)
    up_added = ordered(up_half, swap(up_half, "rep"), group)
    up_added = up_added.transpose(2, 1, 0, 3).reshape(depth, units)
    down_added = ordered(down_half, swap(down_half, "rep"), group)
    down_added = down_added.transpose(1, 0, 2, 3).reshape(units, depth)

    back_sum = scatter_tokens(back_part.astype(jnp.bfloat16), row_count)
    mixed = scatter_tokens(mixed_part.astype(jnp.bfloat16), row_count).astype(jnp.bfloat16)
    scaled_rows = back_sum * norm_gain_vector
    input_gradient_rows = (
        inverse_rms_kept
        * (
            scaled_rows
            - unit_kept_rows * jnp.mean(scaled_rows * unit_kept_rows, axis=-1, keepdims=True)
        )
    ).astype(jnp.bfloat16)
    return (
        mixed,
        input_gradient_rows,
        up_sum + up_added.astype(jnp.float32),
        down_sum + down_added.astype(jnp.float32),
    )


def chosen_body(*args):
    units = args[4].shape[1]
    n_fs = lax.axis_size("fs")
    pairs = lax.axis_size("tp") == 2 and lax.axis_size("rep") == 2 and n_fs % 2 == 0
    return (hidden_body if pairs and units % (128 * n_fs) == 0 else body)(*args)


def solution(mesh):
    return jax.shard_map(
        chosen_body,
        mesh=mesh,
        in_specs=(
            P(("rep", "fs"), None),
            P(("rep", "fs"), None),
            P(("rep", "fs"), None),
            P(),
            P("fs", "tp"),
            P("tp", "fs"),
            P("fs", "tp"),
            P("tp", "fs"),
        ),
        out_specs=(P(("rep", "fs"), None), P(("rep", "fs"), None), P("fs", "tp"), P("tp", "fs")),
        check_vma=False,
    )
```

```python
import functools

import jax
import jax.numpy as jnp
from jax import lax
from jax.experimental import pallas as pl
from jax.experimental.pallas import tpu as pltpu
from jax.sharding import PartitionSpec as P

EPSILON = 1e-06
MESH = pl.DeviceIdType.MESH
TRANSPOSED = (((1,), (1,)), ((), ()))
LEADING = (((0,), (0,)), ((), ()))


def norm_partial_terms(values, norm_gain_vector):
    floats = values.astype(jnp.float32)
    inverse = lax.rsqrt(jnp.mean(floats * floats, axis=-1, keepdims=True) + EPSILON)
    unit_rows = floats * inverse
    normed = (unit_rows * norm_gain_vector).astype(jnp.bfloat16)
    return (inverse, unit_rows, normed)


def squared_relu(pre_act):
    return jnp.square(jax.nn.relu(pre_act)).astype(jnp.bfloat16)


def body(
    x_later, kept_input_rows, cotangent, norm_gain_vector, up_weight, down_weight, up_sum, down_sum
):
    row_count = x_later.shape[0]
    grad_scale = float(row_count * lax.axis_size("rep") * lax.axis_size("fs")) ** (-0.5)
    inv_later, unit_later, normed_later = norm_partial_terms(x_later, norm_gain_vector)
    inverse_rms_kept, unit_kept_rows, normed_kept_rows = norm_partial_terms(
        kept_input_rows, norm_gain_vector
    )
    stacked = jnp.concatenate([normed_kept_rows, normed_later], axis=0)
    up_whole = lax.all_gather(up_weight, "fs", axis=0, tiled=True)
    down_whole = lax.all_gather(down_weight, "fs", axis=1, tiled=True)
    pre_act = jnp.dot(stacked, up_whole, preferred_element_type=jnp.float32)
    pre_saved = pre_act[:row_count]
    hidden_saved = squared_relu(pre_saved)
    hidden_later = squared_relu(pre_act[row_count:])
    mixed_part = jnp.dot(hidden_later, down_whole, preferred_element_type=jnp.float32)
    hidden_grad = lax.dot_general(
        cotangent, down_whole, TRANSPOSED, preferred_element_type=jnp.float32
    )
    pre_grad = (hidden_grad * 2.0 * jax.nn.relu(pre_saved)).astype(jnp.bfloat16)
    back_part = lax.dot_general(pre_grad, up_whole, TRANSPOSED, preferred_element_type=jnp.float32)
    mixed_sum, back_sum = (
        lax.psum(mixed_part.astype(jnp.bfloat16), "tp").astype(jnp.float32),
        lax.psum(back_part.astype(jnp.bfloat16), "tp").astype(jnp.float32),
    )
    mixed = mixed_sum.astype(jnp.bfloat16)
    scaled_rows = back_sum * norm_gain_vector
    input_gradient_rows = (
        inverse_rms_kept
        * (
            scaled_rows
            - unit_kept_rows * jnp.mean(scaled_rows * unit_kept_rows, axis=-1, keepdims=True)
        )
    ).astype(jnp.bfloat16)
    cot_columns, normed_columns = (
        lax.all_to_all(cotangent, "fs", split_axis=1, concat_axis=0, tiled=True),
        lax.all_to_all(normed_kept_rows, "fs", split_axis=1, concat_axis=0, tiled=True),
    )
    columns = normed_columns
    up_grad = grad_scale * lax.dot_general(
        columns,
        lax.all_gather(pre_grad, "fs", axis=0, tiled=True),
        LEADING,
        preferred_element_type=jnp.float32,
    )
    columns = cot_columns
    down_grad = lax.dot_general(
        lax.all_gather(hidden_saved, "fs", axis=0, tiled=True),
        columns,
        LEADING,
        preferred_element_type=jnp.float32,
    )
    up_added, down_added = (
        lax.psum(up_grad.astype(jnp.bfloat16), "rep").astype(jnp.float32),
        lax.psum((down_grad * grad_scale).astype(jnp.bfloat16), "rep").astype(jnp.float32),
    )
    return (mixed, input_gradient_rows, up_sum + up_added, down_sum + down_added)


def swap(values, axis):
    size = lax.axis_size(axis)
    return lax.ppermute(values, axis, [(i, i ^ 1) for i in range(size)])


def own_half(values, axis_index, dim):
    return lax.dynamic_index_in_dim(values, axis_index, dim, keepdims=False)


def line_shift(values, shift):
    size = lax.axis_size("fs")
    outer = size // 2
    return lax.ppermute(
        values, "fs", [(i, ((i // 2 + shift) % outer) * 2 + i % 2) for i in range(size)]
    )


def ordered(first, second, axis_index):
    return jnp.where(axis_index == 0, jnp.stack([first, second]), jnp.stack([second, first]))


def scatter_tokens(partial, rows):
    width = partial.shape[1]
    outer = lax.axis_size("fs") // 2
    blocks = partial.reshape(2, 2, outer, rows // 2, width)
    got = swap(blocks[1], "tp")
    blocks = (blocks[0].astype(jnp.float32) + got.astype(jnp.float32)).astype(jnp.bfloat16)
    got = swap(blocks[1], "fs")
    blocks = (blocks[0].astype(jnp.float32) + got.astype(jnp.float32)).astype(jnp.bfloat16)
    place = lax.axis_index("fs") // 2
    total = own_half(blocks, place, 0).astype(jnp.float32)
    for s in range(1, outer):
        sent = own_half(blocks, (place + s) % outer, 0)
        total = total + line_shift(sent, s).astype(jnp.float32)
    half = total.astype(jnp.bfloat16)
    whole = ordered(half, swap(half, "tp"), lax.axis_index("tp"))
    return whole.reshape(rows, width).astype(jnp.float32)


def gather_kernel(
    n_fs, own, up, down, tok, up_out, down_out,
    line_send, line_recv, pair_send, pair_recv, core_send, core_recv,
    weight_send, weight_recv, local_sem,
):
    rep, fs, core = lax.axis_index("rep"), lax.axis_index("fs"), lax.axis_index("tp")
    outer = n_fs // 2
    place = fs // 2
    pair = fs % 2
    depth, units = up.shape
    own_units = units // n_fs
    part = own_units // 2
    other_pair = (rep, place * 2 + 1 - pair, core)
    other_core = (rep, fs, 1 - core)
    other_rep = (1 - rep, fs, core)

    barrier = pltpu.get_barrier_semaphore()
    peers = [other_core, other_rep]
    peers += [(rep, lax.rem(fs + k, n_fs), core) for k in range(1, n_fs)]
    for peer in peers:
        pl.semaphore_signal(barrier, inc=1, device_id=peer, device_id_type=MESH)
    pl.semaphore_wait(barrier, len(peers))

    def copy(source, target, send, recv, device):
        return pltpu.make_async_remote_copy(
            src_ref=source, dst_ref=target, send_sem=send, recv_sem=recv,
            device_id=device, device_id_type=MESH,
        )

    def slot(other, far, index):
        return tok.at[:, other, far, index]

    def to_line(source, index, way):
        step = 1 if way else -1
        target = (rep, fs + 2 * step, core)
        return copy(source, slot(0, 0, index), line_send.at[way, index], line_recv.at[index], target)

    def to_pair(source, index):
        return copy(
            source, slot(0, 1, index), pair_send.at[index], pair_recv.at[index], other_pair
        )

    def to_core(source, far, index):
        return copy(
            source, slot(1, far, index), core_send.at[far, index], core_recv.at[far, index],
            other_core,
        )

    def up_source(k):
        start = pl.multiple_of(k * own_units + rep * part, part)
        return up.at[:, pl.ds(start, part)]

    def down_source(k):
        start = pl.multiple_of(k * own_units + rep * part, part)
        return down.at[pl.ds(start, part), :]

    def up_slot(k, half):
        return up_out.at[k, :, half * part : (half + 1) * part]

    def down_slot(k, half):
        columns = pl.ds(pl.multiple_of(k * depth, depth), depth)
        return down_out.at[half * part : (half + 1) * part, columns]

    def up_copy(k):
        return copy(
            up_source(k), up_slot(fs, 0), weight_send.at[0, 0, k], weight_recv.at[0, 0, fs],
            (rep, k, core),
        )

    def down_copy(k):
        return copy(
            down_source(k), down_slot(fs, 0), weight_send.at[0, 1, k], weight_recv.at[0, 1, fs],
            (rep, k, core),
        )

    def up_pass(source, k):
        return copy(
            source, up_slot(k, 1), weight_send.at[1, 0, k], weight_recv.at[1, 0, k], other_rep
        )

    def down_pass(source, k):
        return copy(
            source, down_slot(k, 1), weight_send.at[1, 1, k], weight_recv.at[1, 1, k], other_rep
        )

    def landed(target, sem):
        copy(target, target, sem, sem, other_core).wait_recv()

    @pl.when(place > 0)
    def _():
        to_line(own, place, 0).start()

    @pl.when(place < outer - 1)
    def _():
        to_line(own, place, 1).start()

    to_pair(own, place).start()
    to_core(own, 0, place).start()
    keep = [
        pltpu.make_async_copy(own, slot(0, 0, place), local_sem.at[0]),
        pltpu.make_async_copy(up_source(fs), up_slot(fs, 0), local_sem.at[1]),
        pltpu.make_async_copy(down_source(fs), down_slot(fs, 0), local_sem.at[2]),
    ]
    for one in keep:
        one.start()
    up_pass(up_source(fs), fs).start()
    down_pass(down_source(fs), fs).start()
    for k in range(1, n_fs):
        peer = lax.rem(fs + k, n_fs)
        up_copy(peer).start()
        down_copy(peer).start()

    for d in range(1, outer):
        if d == outer - 1:
            for k in range(1, n_fs):
                peer = lax.rem(fs + n_fs - k, n_fs)
                landed(up_slot(peer, 0), weight_recv.at[0, 0, peer])
                up_pass(up_slot(peer, 0), peer).start()
                landed(down_slot(peer, 0), weight_recv.at[0, 1, peer])
                down_pass(down_slot(peer, 0), peer).start()
        for way in range(2):
            index = place - d if way else place + d
            there = index >= 0 if way else index < outer
            more = place < outer - 1 if way else place > 0

            @pl.when(there)
            def _(index=index, way=way, more=more):
                landed(slot(0, 0, index), line_recv.at[index])

                @pl.when(more)
                def _():
                    to_line(slot(0, 0, index), index, way).start()

                to_pair(slot(0, 0, index), index).start()
                to_core(slot(0, 0, index), 0, index).start()

    def pass_pair(index):
        landed(slot(0, 1, index), pair_recv.at[index])
        to_core(slot(0, 1, index), 1, index).start()

    pass_pair(place)
    for d in range(1, outer):
        for way in range(2):
            index = place - d if way else place + d

            @pl.when(index >= 0 if way else index < outer)
            def _(index=index):
                pass_pair(index)

    for one in keep:
        one.wait()
    for k in range(n_fs):
        landed(up_slot(k, 1), weight_recv.at[1, 0, k])
        landed(down_slot(k, 1), weight_recv.at[1, 1, k])
        up_pass(up_slot(k, 0), k).wait_send()
        down_pass(down_slot(k, 0), k).wait_send()
    for k in range(1, n_fs):
        peer = lax.rem(fs + k, n_fs)
        up_copy(peer).wait_send()
        down_copy(peer).wait_send()
    for index in range(outer):
        to_pair(own, index).wait_send()
        for far in range(2):
            landed(slot(1, far, index), core_recv.at[far, index])
            to_core(own, far, index).wait_send()

        @pl.when(jnp.logical_and(index >= place, place > 0))
        def _(index=index):
            to_line(own, index, 0).wait_send()

        @pl.when(jnp.logical_and(index <= place, place < outer - 1))
        def _(index=index):
            to_line(own, index, 1).wait_send()


def gather_all(blocks, up_weight, down_weight):
    n_fs = lax.axis_size("fs")
    outer = n_fs // 2
    arrays, rows, width = blocks.shape
    depth, units = up_weight.shape
    own_units = units // n_fs
    dma = pltpu.SemaphoreType.DMA
    tok, up_own, down_own = pl.pallas_call(
        functools.partial(gather_kernel, n_fs),
        out_shape=(
            jax.ShapeDtypeStruct((arrays, 2, 2, outer, rows, width), blocks.dtype),
            jax.ShapeDtypeStruct((n_fs, depth, own_units), up_weight.dtype),
            jax.ShapeDtypeStruct((own_units, n_fs * depth), down_weight.dtype),
        ),
        in_specs=[pl.BlockSpec(memory_space=pl.ANY)] * 3,
        out_specs=[pl.BlockSpec(memory_space=pl.ANY)] * 3,
        scratch_shapes=[
            dma((2, outer)), dma((outer,)), dma((outer,)), dma((outer,)),
            dma((2, outer)), dma((2, outer)), dma((2, 2, n_fs)), dma((2, 2, n_fs)), dma((3,)),
        ],
        compiler_params=pltpu.CompilerParams(collective_id=0, has_side_effects=True),
    )(blocks, up_weight, down_weight)
    return tok, up_own.reshape(n_fs * depth, own_units), down_own


def hidden_body(
    x_later, kept_input_rows, cotangent, norm_gain_vector, up_weight, down_weight, up_sum, down_sum
):
    row_count, width = x_later.shape
    n_fs = lax.axis_size("fs")
    grad_scale = float(row_count * lax.axis_size("rep") * n_fs) ** (-0.5)
    group = lax.axis_index("rep")
    depth, units = up_weight.shape
    own_units = units // n_fs
    inv_later, unit_later, normed_later = norm_partial_terms(x_later, norm_gain_vector)
    inverse_rms_kept, unit_kept_rows, normed_kept_rows = norm_partial_terms(
        kept_input_rows, norm_gain_vector
    )
    part = own_units // 2
    part = own_units // 2
    core = lax.axis_index("tp")
    blocks = jnp.stack(
        [
            own_half(values.reshape(2, row_count // 2, width), core, 0)
            for values in (normed_kept_rows, cotangent, normed_later)
        ]
    )
    tok, up_own, down_own = gather_all(blocks, up_weight, down_weight)
    normed_saved, cot, normed_next = (tok[i].reshape(-1, width) for i in range(3))

    pre_saved = jnp.dot(normed_saved, up_own, preferred_element_type=jnp.float32)
    hidden_saved = squared_relu(pre_saved)
    hidden_grad = lax.dot_general(cot, down_own, TRANSPOSED, preferred_element_type=jnp.float32)
    pre_grad = (hidden_grad * 2.0 * jax.nn.relu(pre_saved)).astype(jnp.bfloat16)
    up_grad = grad_scale * lax.dot_general(
        normed_saved, pre_grad, LEADING, preferred_element_type=jnp.float32
    )
    down_grad = grad_scale * lax.dot_general(
        hidden_saved, cot, LEADING, preferred_element_type=jnp.float32
    )
    up_got = swap(up_grad[:, part:].astype(jnp.bfloat16), "rep")
    down_got = swap(down_grad[part:].astype(jnp.bfloat16), "rep")
    back_part = lax.dot_general(pre_grad, up_own, TRANSPOSED, preferred_element_type=jnp.float32)
    hidden_later = squared_relu(
        jnp.dot(normed_next, up_own, preferred_element_type=jnp.float32)
    )
    mixed_part = jnp.dot(hidden_later, down_own, preferred_element_type=jnp.float32)
    up_half = (up_grad[:, :part] + up_got.astype(jnp.float32)).astype(jnp.bfloat16)
    down_half = (down_grad[:part] + down_got.astype(jnp.float32)).astype(jnp.bfloat16)
    up_half = lax.all_to_all(up_half.reshape(n_fs, depth, part), "fs", 0, 0, tiled=True)
    down_half = down_half.reshape(part, n_fs, depth).transpose(1, 0, 2)
    down_half = lax.all_to_all(down_half, "fs", 0, 0, tiled=True)
    up_added = ordered(up_half, swap(up_half, "rep"), group)
    up_added = up_added.transpose(2, 1, 0, 3).reshape(depth, units)
    down_added = ordered(down_half, swap(down_half, "rep"), group)
    down_added = down_added.transpose(1, 0, 2, 3).reshape(units, depth)

    back_sum = scatter_tokens(back_part.astype(jnp.bfloat16), row_count)
    mixed = scatter_tokens(mixed_part.astype(jnp.bfloat16), row_count).astype(jnp.bfloat16)
    scaled_rows = back_sum * norm_gain_vector
    input_gradient_rows = (
        inverse_rms_kept
        * (
            scaled_rows
            - unit_kept_rows * jnp.mean(scaled_rows * unit_kept_rows, axis=-1, keepdims=True)
        )
    ).astype(jnp.bfloat16)
    return (
        mixed,
        input_gradient_rows,
        up_sum + up_added.astype(jnp.float32),
        down_sum + down_added.astype(jnp.float32),
    )


def chosen_body(*args):
    units = args[4].shape[1]
    n_fs = lax.axis_size("fs")
    pairs = lax.axis_size("tp") == 2 and lax.axis_size("rep") == 2 and n_fs % 2 == 0
    return (hidden_body if pairs and units % (128 * n_fs) == 0 else body)(*args)


def solution(mesh):
    return jax.shard_map(
        chosen_body,
        mesh=mesh,
        in_specs=(
            P(("rep", "fs"), None),
            P(("rep", "fs"), None),
            P(("rep", "fs"), None),
            P(),
            P("fs", "tp"),
            P("tp", "fs"),
            P("fs", "tp"),
            P("tp", "fs"),
        ),
        out_specs=(P(("rep", "fs"), None), P(("rep", "fs"), None), P("fs", "tp"), P("tp", "fs")),
        check_vma=False,
    )
```

```python
import functools

import jax
import jax.numpy as jnp
from jax import lax
from jax.experimental import pallas as pl
from jax.experimental.pallas import tpu as pltpu
from jax.sharding import PartitionSpec as P

EPSILON = 1e-06
MESH = pl.DeviceIdType.MESH
TRANSPOSED = (((1,), (1,)), ((), ()))
LEADING = (((0,), (0,)), ((), ()))


def norm_partial_terms(values, norm_gain_vector):
    floats = values.astype(jnp.float32)
    inverse = lax.rsqrt(jnp.mean(floats * floats, axis=-1, keepdims=True) + EPSILON)
    unit_rows = floats * inverse
    normed = (unit_rows * norm_gain_vector).astype(jnp.bfloat16)
    return (inverse, unit_rows, normed)


def squared_relu(pre_act):
    return jnp.square(jax.nn.relu(pre_act)).astype(jnp.bfloat16)


def body(
    x_later, kept_input_rows, cotangent, norm_gain_vector, up_weight, down_weight, up_sum, down_sum
):
    row_count = x_later.shape[0]
    grad_scale = float(row_count * lax.axis_size("rep") * lax.axis_size("fs")) ** (-0.5)
    inv_later, unit_later, normed_later = norm_partial_terms(x_later, norm_gain_vector)
    inverse_rms_kept, unit_kept_rows, normed_kept_rows = norm_partial_terms(
        kept_input_rows, norm_gain_vector
    )
    stacked = jnp.concatenate([normed_kept_rows, normed_later], axis=0)
    up_whole = lax.all_gather(up_weight, "fs", axis=0, tiled=True)
    down_whole = lax.all_gather(down_weight, "fs", axis=1, tiled=True)
    pre_act = jnp.dot(stacked, up_whole, preferred_element_type=jnp.float32)
    pre_saved = pre_act[:row_count]
    hidden_saved = squared_relu(pre_saved)
    hidden_later = squared_relu(pre_act[row_count:])
    mixed_part = jnp.dot(hidden_later, down_whole, preferred_element_type=jnp.float32)
    hidden_grad = lax.dot_general(
        cotangent, down_whole, TRANSPOSED, preferred_element_type=jnp.float32
    )
    pre_grad = (hidden_grad * 2.0 * jax.nn.relu(pre_saved)).astype(jnp.bfloat16)
    back_part = lax.dot_general(pre_grad, up_whole, TRANSPOSED, preferred_element_type=jnp.float32)
    mixed_sum, back_sum = (
        lax.psum(mixed_part.astype(jnp.bfloat16), "tp").astype(jnp.float32),
        lax.psum(back_part.astype(jnp.bfloat16), "tp").astype(jnp.float32),
    )
    mixed = mixed_sum.astype(jnp.bfloat16)
    scaled_rows = back_sum * norm_gain_vector
    input_gradient_rows = (
        inverse_rms_kept
        * (
            scaled_rows
            - unit_kept_rows * jnp.mean(scaled_rows * unit_kept_rows, axis=-1, keepdims=True)
        )
    ).astype(jnp.bfloat16)
    cot_columns, normed_columns = (
        lax.all_to_all(cotangent, "fs", split_axis=1, concat_axis=0, tiled=True),
        lax.all_to_all(normed_kept_rows, "fs", split_axis=1, concat_axis=0, tiled=True),
    )
    columns = normed_columns
    up_grad = grad_scale * lax.dot_general(
        columns,
        lax.all_gather(pre_grad, "fs", axis=0, tiled=True),
        LEADING,
        preferred_element_type=jnp.float32,
    )
    columns = cot_columns
    down_grad = lax.dot_general(
        lax.all_gather(hidden_saved, "fs", axis=0, tiled=True),
        columns,
        LEADING,
        preferred_element_type=jnp.float32,
    )
    up_added, down_added = (
        lax.psum(up_grad.astype(jnp.bfloat16), "rep").astype(jnp.float32),
        lax.psum((down_grad * grad_scale).astype(jnp.bfloat16), "rep").astype(jnp.float32),
    )
    return (mixed, input_gradient_rows, up_sum + up_added, down_sum + down_added)


def swap(values, axis):
    size = lax.axis_size(axis)
    return lax.ppermute(values, axis, [(i, i ^ 1) for i in range(size)])


def own_half(values, axis_index, dim):
    return lax.dynamic_index_in_dim(values, axis_index, dim, keepdims=False)


def line_shift(values, shift):
    size = lax.axis_size("fs")
    outer = size // 2
    return lax.ppermute(
        values, "fs", [(i, ((i // 2 + shift) % outer) * 2 + i % 2) for i in range(size)]
    )


def ordered(first, second, axis_index):
    return jnp.where(axis_index == 0, jnp.stack([first, second]), jnp.stack([second, first]))


def core_sum(partial, rows):
    outer = lax.axis_size("fs") // 2
    blocks = partial.astype(jnp.bfloat16).reshape(2, 2, outer, rows // 2, partial.shape[1])
    got = swap(blocks[1], "tp")
    return (blocks[0].astype(jnp.float32) + got.astype(jnp.float32)).astype(jnp.bfloat16)


def scatter_tokens(blocks):
    outer = lax.axis_size("fs") // 2
    got = swap(blocks[1], "fs")
    blocks = (blocks[0].astype(jnp.float32) + got.astype(jnp.float32)).astype(jnp.bfloat16)
    place = lax.axis_index("fs") // 2
    total = own_half(blocks, place, 0).astype(jnp.float32)
    for s in range(1, outer):
        sent = own_half(blocks, (place + s) % outer, 0)
        total = total + line_shift(sent, s).astype(jnp.float32)
    half = total.astype(jnp.bfloat16)
    whole = ordered(half, swap(half, "tp"), lax.axis_index("tp"))
    return whole.reshape(-1, half.shape[1]).astype(jnp.float32)


def gather_kernel(
    n_fs, own, up, down, tok, up_out, down_out,
    line_send, line_recv, pair_send, pair_recv, core_send, core_recv,
    weight_send, weight_recv, local_sem,
):
    rep, fs, core = lax.axis_index("rep"), lax.axis_index("fs"), lax.axis_index("tp")
    outer = n_fs // 2
    place = fs // 2
    pair = fs % 2
    depth, units = up.shape
    own_units = units // n_fs
    part = own_units // 2
    other_pair = (rep, place * 2 + 1 - pair, core)
    other_core = (rep, fs, 1 - core)
    other_rep = (1 - rep, fs, core)

    barrier = pltpu.get_barrier_semaphore()
    peers = [other_core, other_rep]
    peers += [(rep, lax.rem(fs + k, n_fs), core) for k in range(1, n_fs)]
    for peer in peers:
        pl.semaphore_signal(barrier, inc=1, device_id=peer, device_id_type=MESH)
    pl.semaphore_wait(barrier, len(peers))

    def copy(source, target, send, recv, device):
        return pltpu.make_async_remote_copy(
            src_ref=source, dst_ref=target, send_sem=send, recv_sem=recv,
            device_id=device, device_id_type=MESH,
        )

    def slot(other, far, index):
        return tok.at[:, other, far, index]

    def to_line(source, index, way):
        step = 1 if way else -1
        target = (rep, fs + 2 * step, core)
        return copy(source, slot(0, 0, index), line_send.at[way, index], line_recv.at[index], target)

    def to_pair(source, index):
        return copy(
            source, slot(0, 1, index), pair_send.at[index], pair_recv.at[index], other_pair
        )

    def to_core(source, far, index):
        return copy(
            source, slot(1, far, index), core_send.at[far, index], core_recv.at[far, index],
            other_core,
        )

    def up_source(k):
        start = pl.multiple_of(k * own_units + rep * part, part)
        return up.at[:, pl.ds(start, part)]

    def down_source(k):
        start = pl.multiple_of(k * own_units + rep * part, part)
        return down.at[pl.ds(start, part), :]

    def up_slot(k, half):
        return up_out.at[k, :, half * part : (half + 1) * part]

    def down_slot(k, half):
        columns = pl.ds(pl.multiple_of(k * depth, depth), depth)
        return down_out.at[half * part : (half + 1) * part, columns]

    def up_copy(k):
        return copy(
            up_source(k), up_slot(fs, 0), weight_send.at[0, 0, k], weight_recv.at[0, 0, fs],
            (rep, k, core),
        )

    def down_copy(k):
        return copy(
            down_source(k), down_slot(fs, 0), weight_send.at[0, 1, k], weight_recv.at[0, 1, fs],
            (rep, k, core),
        )

    def up_pass(source, k):
        return copy(
            source, up_slot(k, 1), weight_send.at[1, 0, k], weight_recv.at[1, 0, k], other_rep
        )

    def down_pass(source, k):
        return copy(
            source, down_slot(k, 1), weight_send.at[1, 1, k], weight_recv.at[1, 1, k], other_rep
        )

    def landed(target, sem):
        copy(target, target, sem, sem, other_core).wait_recv()

    @pl.when(place > 0)
    def _():
        to_line(own, place, 0).start()

    @pl.when(place < outer - 1)
    def _():
        to_line(own, place, 1).start()

    to_pair(own, place).start()
    to_core(own, 0, place).start()
    keep = [
        pltpu.make_async_copy(own, slot(0, 0, place), local_sem.at[0]),
        pltpu.make_async_copy(up_source(fs), up_slot(fs, 0), local_sem.at[1]),
        pltpu.make_async_copy(down_source(fs), down_slot(fs, 0), local_sem.at[2]),
    ]
    for one in keep:
        one.start()
    up_pass(up_source(fs), fs).start()
    down_pass(down_source(fs), fs).start()
    for k in range(1, n_fs):
        peer = lax.rem(fs + k, n_fs)
        up_copy(peer).start()
        down_copy(peer).start()

    for d in range(1, outer):
        if d == outer - 1:
            for k in range(1, n_fs):
                peer = lax.rem(fs + n_fs - k, n_fs)
                landed(up_slot(peer, 0), weight_recv.at[0, 0, peer])
                up_pass(up_slot(peer, 0), peer).start()
                landed(down_slot(peer, 0), weight_recv.at[0, 1, peer])
                down_pass(down_slot(peer, 0), peer).start()
        for way in range(2):
            index = place - d if way else place + d
            there = index >= 0 if way else index < outer
            more = place < outer - 1 if way else place > 0

            @pl.when(there)
            def _(index=index, way=way, more=more):
                landed(slot(0, 0, index), line_recv.at[index])

                @pl.when(more)
                def _():
                    to_line(slot(0, 0, index), index, way).start()

                to_pair(slot(0, 0, index), index).start()
                to_core(slot(0, 0, index), 0, index).start()

    def pass_pair(index):
        landed(slot(0, 1, index), pair_recv.at[index])
        to_core(slot(0, 1, index), 1, index).start()

    pass_pair(place)
    for d in range(1, outer):
        for way in range(2):
            index = place - d if way else place + d

            @pl.when(index >= 0 if way else index < outer)
            def _(index=index):
                pass_pair(index)

    for one in keep:
        one.wait()
    for k in range(n_fs):
        landed(up_slot(k, 1), weight_recv.at[1, 0, k])
        landed(down_slot(k, 1), weight_recv.at[1, 1, k])
        up_pass(up_slot(k, 0), k).wait_send()
        down_pass(down_slot(k, 0), k).wait_send()
    for k in range(1, n_fs):
        peer = lax.rem(fs + k, n_fs)
        up_copy(peer).wait_send()
        down_copy(peer).wait_send()
    for index in range(outer):
        to_pair(own, index).wait_send()
        for far in range(2):
            landed(slot(1, far, index), core_recv.at[far, index])
            to_core(own, far, index).wait_send()

        @pl.when(jnp.logical_and(index >= place, place > 0))
        def _(index=index):
            to_line(own, index, 0).wait_send()

        @pl.when(jnp.logical_and(index <= place, place < outer - 1))
        def _(index=index):
            to_line(own, index, 1).wait_send()


def gather_all(blocks, up_weight, down_weight):
    n_fs = lax.axis_size("fs")
    outer = n_fs // 2
    arrays, rows, width = blocks.shape
    depth, units = up_weight.shape
    own_units = units // n_fs
    dma = pltpu.SemaphoreType.DMA
    tok, up_own, down_own = pl.pallas_call(
        functools.partial(gather_kernel, n_fs),
        out_shape=(
            jax.ShapeDtypeStruct((arrays, 2, 2, outer, rows, width), blocks.dtype),
            jax.ShapeDtypeStruct((n_fs, depth, own_units), up_weight.dtype),
            jax.ShapeDtypeStruct((own_units, n_fs * depth), down_weight.dtype),
        ),
        in_specs=[pl.BlockSpec(memory_space=pl.ANY)] * 3,
        out_specs=[pl.BlockSpec(memory_space=pl.ANY)] * 3,
        scratch_shapes=[
            dma((2, outer)), dma((outer,)), dma((outer,)), dma((outer,)),
            dma((2, outer)), dma((2, outer)), dma((2, 2, n_fs)), dma((2, 2, n_fs)), dma((3,)),
        ],
        compiler_params=pltpu.CompilerParams(collective_id=0, has_side_effects=True),
    )(blocks, up_weight, down_weight)
    return tok, up_own.reshape(n_fs * depth, own_units), down_own


def add_kernel(own, got, total, out):
    first = lax.axis_index("rep") == 0
    parts, _, part = own.shape
    for k in range(parts):
        mine, other = own[k].astype(jnp.float32), got[k].astype(jnp.float32)
        left = slice(2 * k * part, (2 * k + 1) * part)
        right = slice((2 * k + 1) * part, (2 * k + 2) * part)
        out[:, left] = total[:, left] + jnp.where(first, mine, other)
        out[:, right] = total[:, right] + jnp.where(first, other, mine)


def add_up(own, got, total):
    parts, depth, part = own.shape
    rows = depth // 4
    blocks = pl.BlockSpec((parts, rows, part), lambda i: (0, i, 0))
    whole = pl.BlockSpec((rows, total.shape[1]), lambda i: (i, 0))
    return pl.pallas_call(
        add_kernel,
        grid=(4,),
        out_shape=jax.ShapeDtypeStruct(total.shape, total.dtype),
        in_specs=[blocks, blocks, whole],
        out_specs=whole,
        cost_estimate=pl.CostEstimate(
            flops=2 * total.size, bytes_accessed=10 * total.size, transcendentals=0
        ),
    )(own, got, total)


def hidden_body(
    x_later, kept_input_rows, cotangent, norm_gain_vector, up_weight, down_weight, up_sum, down_sum
):
    row_count, width = x_later.shape
    n_fs = lax.axis_size("fs")
    grad_scale = float(row_count * lax.axis_size("rep") * n_fs) ** (-0.5)
    group = lax.axis_index("rep")
    depth, units = up_weight.shape
    own_units = units // n_fs
    inv_later, unit_later, normed_later = norm_partial_terms(x_later, norm_gain_vector)
    inverse_rms_kept, unit_kept_rows, normed_kept_rows = norm_partial_terms(
        kept_input_rows, norm_gain_vector
    )
    part = own_units // 2
    part = own_units // 2
    core = lax.axis_index("tp")
    blocks = jnp.stack(
        [
            own_half(values.reshape(2, row_count // 2, width), core, 0)
            for values in (normed_kept_rows, cotangent, normed_later)
        ]
    )
    tok, up_own, down_own = gather_all(blocks, up_weight, down_weight)
    normed_saved, cot, normed_next = (tok[i].reshape(-1, width) for i in range(3))

    pre_saved = jnp.dot(normed_saved, up_own, preferred_element_type=jnp.float32)
    hidden_saved = squared_relu(pre_saved)
    hidden_grad = lax.dot_general(cot, down_own, TRANSPOSED, preferred_element_type=jnp.float32)
    pre_grad = (hidden_grad * 2.0 * jax.nn.relu(pre_saved)).astype(jnp.bfloat16)
    back_part = lax.dot_general(pre_grad, up_own, TRANSPOSED, preferred_element_type=jnp.float32)
    back_blocks = core_sum(back_part, row_count)
    hidden_later = squared_relu(
        jnp.dot(normed_next, up_own, preferred_element_type=jnp.float32)
    )
    mixed_part = jnp.dot(hidden_later, down_own, preferred_element_type=jnp.float32)
    mixed_blocks = core_sum(mixed_part, row_count)
    pre_grad, hidden_saved, mixed_blocks = lax.optimization_barrier(
        (pre_grad, hidden_saved, mixed_blocks)
    )
    up_grad = grad_scale * lax.dot_general(
        normed_saved, pre_grad, LEADING, preferred_element_type=jnp.float32
    )
    down_grad = grad_scale * lax.dot_general(
        hidden_saved, cot, LEADING, preferred_element_type=jnp.float32
    )
    up_got = swap(up_grad[:, part:].astype(jnp.bfloat16), "rep")
    down_got = swap(down_grad[part:].astype(jnp.bfloat16), "rep")
    up_half = (up_grad[:, :part] + up_got.astype(jnp.float32)).astype(jnp.bfloat16)
    down_half = (down_grad[:part] + down_got.astype(jnp.float32)).astype(jnp.bfloat16)
    up_half = lax.all_to_all(up_half.reshape(n_fs, depth, part), "fs", 0, 0, tiled=True)
    down_half = down_half.reshape(part, n_fs, depth).transpose(1, 0, 2)
    down_half = lax.all_to_all(down_half, "fs", 0, 0, tiled=True)
    up_total = add_up(up_half, swap(up_half, "rep"), up_sum)
    down_added = ordered(down_half, swap(down_half, "rep"), group)
    down_added = down_added.transpose(1, 0, 2, 3).reshape(units, depth)

    back_sum = scatter_tokens(back_blocks)
    mixed = scatter_tokens(mixed_blocks).astype(jnp.bfloat16)
    scaled_rows = back_sum * norm_gain_vector
    input_gradient_rows = (
        inverse_rms_kept
        * (
            scaled_rows
            - unit_kept_rows * jnp.mean(scaled_rows * unit_kept_rows, axis=-1, keepdims=True)
        )
    ).astype(jnp.bfloat16)
    return (
        mixed,
        input_gradient_rows,
        up_total,
        down_sum + down_added.astype(jnp.float32),
    )


def chosen_body(*args):
    units = args[4].shape[1]
    n_fs = lax.axis_size("fs")
    pairs = lax.axis_size("tp") == 2 and lax.axis_size("rep") == 2 and n_fs % 2 == 0
    return (hidden_body if pairs and units % (256 * n_fs) == 0 else body)(*args)


def solution(mesh):
    return jax.shard_map(
        chosen_body,
        mesh=mesh,
        in_specs=(
            P(("rep", "fs"), None),
            P(("rep", "fs"), None),
            P(("rep", "fs"), None),
            P(),
            P("fs", "tp"),
            P("tp", "fs"),
            P("fs", "tp"),
            P("tp", "fs"),
        ),
        out_specs=(P(("rep", "fs"), None), P(("rep", "fs"), None), P("fs", "tp"), P("tp", "fs")),
        check_vma=False,
    )
```
